32 devices in a mesh: sp: 16 (over z, y, core), tp: 2 (over x).
Axes of the slice: x: 2, y: 2, z: 4, core: 2. Of those that a mesh axis runs over, the one named last changes fastest.
Arguments:
- stream: bfloat16 [2048, 2048], P('sp', 'tp'), may hold values from -52 to 52
- norm_gain: float32 [2, 2048], replicated, may hold values from 0.1 to 1.9
- value_weight: bfloat16 [4096, 1024], P('sp', 'tp'), may hold values from -0.125 to 0.125
- gate_weight: bfloat16 [4096, 1024], P('sp', 'tp'), may hold values from -0.125 to 0.125
- conv_taps: float32 [2, 31, 1024], replicated, may hold values from -3 to 3
- ln_gain: float32 [2, 1024], replicated, may hold values from 0.1 to 1.9
- ln_bias: float32 [2, 1024], replicated, may hold values from -3 to 3
- out_weight: bfloat16 [1024, 4096], P('tp', 'sp'), may hold values from -0.1875 to 0.1875
- final_gain: float32 [2048], replicated, may hold values from 0.1 to 1.9
Outputs:
- result: bfloat16 [2048, 2048], P('sp', 'tp')
The draws below stay inside these ranges and needn't reach their ends.
All inputs are finite; a program needn't handle non-finite values.
Results may differ from the reference program's by a relative error of at most 0.014.
Values may be sent and summed in bfloat16 or wider, within the bound.
A program may use at most 64 MiB of HBM per device.

```python
import math
import jax
import jax.numpy as jnp
from jax import lax

D = 2048
C = 1024
KW = 31
LAYERS = 2
TOKENS = 2048
N_TP = 2


def draw_stream(key, part):
    key_values, key_rows, key_cols = jax.random.split(key, 3)
    column_place = jnp.arange(D, dtype=jnp.float32) / D - 0.5
    col_scale = jnp.exp(jnp.log(8.0) * column_place + jax.random.uniform(key_cols, (D,), jnp.float32, -0.35, 0.35))
    row_scale = jnp.exp(jax.random.uniform(key_rows, (TOKENS, 1), jnp.float32, -1.15, 1.15))
    values = jnp.clip(jax.random.normal(key_values, (TOKENS, D), jnp.float32), -4.0, 4.0)
    return (values * row_scale * col_scale).astype(jnp.bfloat16)


def draw_conv_taps(key, part):
    key_values, key_chans = jax.random.split(key)
    chan_place = jnp.arange(C, dtype=jnp.float32) / C - 0.5
    chan_scale = jnp.exp(jnp.log(6.0) * chan_place + jax.random.uniform(key_chans, (C,), jnp.float32, -0.35, 0.35))
    values = jnp.clip(jax.random.normal(key_values, (LAYERS, KW, C), jnp.float32), -4.0, 4.0)
    return (values * chan_scale / math.sqrt(KW)).astype(jnp.float32)


def level_of(stream_key, shape, shards, smallest, high):
    factor_of = 1.0
    for dim, blocks in shards:
        draws = jax.random.uniform(jax.random.fold_in(jax.random.fold_in(stream_key, 6), dim), (blocks,), jnp.float32, smallest / len(shards), high / len(shards))
        factor_of = factor_of * jnp.repeat(jnp.exp(draws), shape[dim] // blocks).reshape((-1,) + (1,) * (len(shape) - 1 - dim))
    return factor_of


def gaussian(own_key, dims, deviation, most, shards=(), held_as=jnp.bfloat16):
    factor_of = level_of(own_key, dims, shards, -0.22, 0.18) if shards else 1.0
    result = jax.random.normal(own_key, dims, jnp.float32) * deviation * factor_of
    return jnp.minimum(jnp.maximum(result, -most), most).astype(held_as)


def setup_inputs(seed: int = 0) -> dict:
    arg_keys = jax.random.split(jax.random.key(seed), 10)
    stream = draw_stream(jax.random.fold_in(arg_keys[9], 71), 0)
    norm_gain = jnp.clip(1.0 + 0.18 * jax.random.normal(arg_keys[1], (LAYERS, D), jnp.float32), 0.1, 1.9)
    value_weight = gaussian(arg_keys[2], (LAYERS * D, C), D ** -0.5, 0.125, ((0, 16), (1, 2)))
    gate_weight = gaussian(arg_keys[3], (LAYERS * D, C), D ** -0.5, 0.125, ((0, 16), (1, 2)))
    conv_taps = draw_conv_taps(jax.random.fold_in(arg_keys[9], 71), 0)
    ln_gain = jnp.clip(1.0 + 0.18 * jax.random.normal(arg_keys[5], (LAYERS, C), jnp.float32), 0.1, 1.9)
    ln_bias = gaussian(arg_keys[6], (LAYERS, C), 0.5, 3.0, (), jnp.float32)
    out_weight = gaussian(arg_keys[7], (C, LAYERS * D), C ** -0.5, 0.1875, ((0, 2), (1, 16)))
    final_gain = jnp.clip(1.0 + 0.18 * jax.random.normal(arg_keys[8], (D,), jnp.float32), 0.1, 1.9)
    return {"stream": stream, "norm_gain": norm_gain, "value_weight": value_weight, "gate_weight": gate_weight, "conv_taps": conv_taps, "ln_gain": ln_gain, "ln_bias": ln_bias, "out_weight": out_weight, "final_gain": final_gain}


EPS = 1e-06

def valid_conv(extended, tap_table):
    length = extended.shape[0] - (KW - 1)
    running = tap_table[0] * extended[0:length]
    for tap_index in range(1, KW):
        running = running + tap_table[tap_index] * extended[tap_index:tap_index + length]
    return running

def reference(stream, norm_gain, value_weight, gate_weight, conv_taps, ln_gain, ln_bias, out_weight, final_gain):
    value_all = value_weight.reshape(D, LAYERS, C)
    gate_all = gate_weight.reshape(D, LAYERS, C)
    out_all = out_weight.reshape(C, D, LAYERS)
    block_width = C // N_TP
    current = stream
    for layer_index in range(LAYERS):
        current32 = current.astype(jnp.float32)
        scale = lax.rsqrt(lax.optimization_barrier(jnp.sum(current32 * current32, axis=1, keepdims=True)) / D + EPS)
        normed = (current32 * scale * norm_gain[layer_index]).astype(jnp.bfloat16)
        value_proj = jnp.dot(normed, value_all[:, layer_index], preferred_element_type=jnp.float32)
        gate_proj = jnp.dot(normed, gate_all[:, layer_index], preferred_element_type=jnp.float32)
        glu_out = value_proj * jax.nn.sigmoid(gate_proj)
        extended = jnp.concatenate([jnp.zeros((KW - 1, C), jnp.float32), glu_out], axis=0)
        conv_out = valid_conv(extended, conv_taps[layer_index])
        row_mean = lax.optimization_barrier(jnp.sum(conv_out, axis=1, keepdims=True)) / C
        row_var = lax.optimization_barrier(jnp.sum(conv_out * conv_out, axis=1, keepdims=True)) / C - row_mean * row_mean
        active = jax.nn.silu((conv_out - row_mean) * lax.rsqrt(row_var + EPS) * ln_gain[layer_index] + ln_bias[layer_index]).astype(jnp.bfloat16)
        branch = jnp.zeros((current.shape[0], D), jnp.float32)
        for block_index in range(N_TP):
            low = block_index * block_width
            partial_value = jnp.dot(active[:, low:low + block_width], out_all[low:low + block_width, :, layer_index], preferred_element_type=jnp.float32)
            branch = branch + lax.optimization_barrier(partial_value.astype(jnp.bfloat16)).astype(jnp.float32)
        current = (current32 + branch).astype(jnp.bfloat16)
    final32 = current.astype(jnp.float32)
    squares = lax.optimization_barrier(jnp.sum(final32 * final32, axis=1, keepdims=True))
    return (final32 * lax.rsqrt(squares / D + EPS) * final_gain).astype(jnp.bfloat16)
```

```python
import functools

import jax
import jax.numpy as jnp
from jax import lax
from jax.experimental import pallas as pl
from jax.experimental.pallas import tpu as pltpu
from jax.sharding import PartitionSpec as P

D = 2048
C = 1024
KW = 31
LAYERS = 2


EPS = 1e-06


def from_behind(value, axis, steps):
    count = lax.axis_size(axis)
    first, last = (max(0, -steps), min(count, count - steps))
    return lax.ppermute(value, axis, [(source, source + steps) for source in range(first, last)])


def valid_conv(extended, tap_table):
    length = extended.shape[0] - (KW - 1)
    running = tap_table[0] * extended[0:length]
    for tap_index in range(1, KW):
        running = running + tap_table[tap_index] * extended[tap_index : tap_index + length]
    return running


def local(
    stream,
    norm_gain,
    value_weight,
    gate_weight,
    conv_taps,
    ln_gain,
    ln_bias,
    out_weight,
    final_gain,
):
    tokens_here = stream.shape[0]
    columns = stream.shape[1]
    channels = value_weight.shape[1]
    rim_rows = KW - 1
    tp_index = lax.axis_index("tp")
    my_taps = lax.dynamic_slice_in_dim(conv_taps, tp_index * channels, channels, 2)
    my_ln_gain = lax.dynamic_slice_in_dim(ln_gain, tp_index * channels, channels, 1)
    my_ln_bias = lax.dynamic_slice_in_dim(ln_bias, tp_index * channels, channels, 1)
    my_final = lax.dynamic_slice_in_dim(final_gain, tp_index * columns, columns, 0)
    value_all, gate_all, out_all = (
        lax.all_gather(value_weight, "sp", axis=0, tiled=True),
        lax.all_gather(gate_weight, "sp", axis=0, tiled=True),
        lax.all_gather(out_weight, "sp", axis=1, tiled=True),
    )
    value_all = value_all.reshape(D, LAYERS, channels)
    gate_all = gate_all.reshape(D, LAYERS, channels)
    out_all = out_all.reshape(channels, D, LAYERS)
    earlier = from_behind(stream[-LAYERS * rim_rows :], "sp", 1)
    current = jnp.concatenate([earlier, stream], axis=0)
    for layer_index in range(LAYERS):
        prefix = (LAYERS - layer_index) * rim_rows
        gathered = lax.all_gather(current, "tp", axis=1, tiled=True)
        gathered32 = gathered.astype(jnp.float32)
        scale = lax.rsqrt(jnp.sum(gathered32 * gathered32, axis=1, keepdims=True) / D + EPS)
        run_normed = (gathered32 * scale * norm_gain[layer_index]).astype(jnp.bfloat16)
        value_proj = jnp.dot(
            run_normed, value_all[:, layer_index], preferred_element_type=jnp.float32
        )
        gate_proj = jnp.dot(
            run_normed, gate_all[:, layer_index], preferred_element_type=jnp.float32
        )
        glu_out = value_proj * jax.nn.sigmoid(gate_proj)
        positions = (
            lax.axis_index("sp") * tokens_here - prefix + lax.iota(jnp.int32, current.shape[0])
        )
        extended = jnp.where((positions >= 0)[:, None], glu_out, 0.0)
        residual = current[rim_rows:].astype(jnp.float32)
        conv_out = valid_conv(extended, my_taps[layer_index])
        first_sums, square_sums = lax.psum(
            (jnp.sum(conv_out, axis=1), jnp.sum(conv_out * conv_out, axis=1)), "tp"
        )
        row_mean = (first_sums / C)[:, None]
        row_var = (square_sums / C)[:, None] - row_mean * row_mean
        run_active = jax.nn.silu(
            (conv_out - row_mean) * lax.rsqrt(row_var + EPS) * my_ln_gain[layer_index]
            + my_ln_bias[layer_index]
        ).astype(jnp.bfloat16)
        partial_value = jnp.dot(
            run_active, out_all[:, :, layer_index], preferred_element_type=jnp.float32
        )
        summed = lax.psum_scatter(
            partial_value.astype(jnp.bfloat16), "tp", scatter_dimension=1, tiled=True
        ).astype(jnp.float32)
        current = (residual + summed).astype(jnp.bfloat16)
    final32 = current.astype(jnp.float32)
    squares = lax.psum(jnp.sum(final32 * final32, axis=1), "tp")
    return (final32 * lax.rsqrt(squares[:, None] / D + EPS) * my_final).astype(jnp.bfloat16)


MESH = pl.DeviceIdType.MESH
HALO = 32
UP, DOWN, SIDE, CORE = range(4)
ITEMS = 3 * LAYERS


def fused_kernel(
    n, x_ref, ng_ref, v_ref, g_ref, taps_ref, lng_ref, lnb_ref, o_ref, fg_ref, out_ref,
    vg, ob, xf, xn, nb, ext, cv, act, part, rpart, st, rst,
    ssem, rsem, xsem, hsem, tsem, psem,
):
    levels = n // 4
    sp = lax.axis_index("sp")
    tp = lax.axis_index("tp")
    z, y, core = sp // 4, (sp // 2) % 2, sp % 2
    peer = 1 - tp
    rows, cols = x_ref.shape
    depth = v_ref.shape[0] // LAYERS
    ch = v_ref.shape[1]
    width = o_ref.shape[1] // LAYERS
    has_up, has_down = z < levels - 1, z > 0
    target = {UP: sp + 4, DOWN: sp - 4, SIDE: sp + 2 - 4 * y, CORE: sp + 1 - 2 * core}

    def slot(k, src):
        layer, kind = divmod(k, 3)
        return ob.at[layer, src] if kind == 2 else vg.at[layer * 2 + kind, src]

    def copy(k, src, way):
        return pltpu.make_async_remote_copy(
            src_ref=slot(k, src), dst_ref=slot(k, src),
            send_sem=ssem.at[k, way, src], recv_sem=rsem.at[k, src],
            device_id={"sp": target[way], "tp": tp}, device_id_type=MESH)

    def index(zz, yy, cc):
        return (zz * 2 + yy) * 2 + cc

    def from_below(d):
        return index(z - d, y, core)

    def from_above(d):
        return index(z + d, y, core)

    def own(k, act_on):
        act_on(k, sp, SIDE)
        pl.when(has_up)(lambda: act_on(k, sp, UP))
        pl.when(has_down)(lambda: act_on(k, sp, DOWN))
        act_on(k, sp, CORE)

    def line(k, act_on, wait):
        for d in range(1, levels):
            @pl.when(z - d >= 0)
            def _():
                if wait:
                    copy(k, from_below(d), UP).wait_recv()
                act_on(k, from_below(d), SIDE)
                pl.when(has_up)(lambda: act_on(k, from_below(d), UP))
                act_on(k, from_below(d), CORE)

            @pl.when(z + d < levels)
            def _():
                if wait:
                    copy(k, from_above(d), DOWN).wait_recv()
                act_on(k, from_above(d), SIDE)
                pl.when(has_down)(lambda: act_on(k, from_above(d), DOWN))
                act_on(k, from_above(d), CORE)

    def across(k, act_on, wait):
        def one(src):
            if wait:
                copy(k, src, SIDE).wait_recv()
            act_on(k, src, CORE)

        one(index(z, 1 - y, core))
        for d in range(1, levels):
            pl.when(z - d >= 0)(lambda: one(index(z - d, 1 - y, core)))
            pl.when(z + d < levels)(lambda: one(index(z + d, 1 - y, core)))

    def other_core(k):
        for zz in range(levels):
            for yy in range(2):
                copy(k, index(zz, yy, 1 - core), CORE).wait_recv()

    def start(k, src, way):
        copy(k, src, way).start()

    def finish(k, src, way):
        copy(k, src, way).wait_send()

    def to_peer(src, dst, sems):
        return pltpu.make_async_remote_copy(
            src_ref=src, dst_ref=dst, send_sem=sems[0], recv_sem=sems[1],
            device_id={"sp": sp, "tp": peer}, device_id_type=MESH)

    def halo(layer):
        return pltpu.make_async_remote_copy(
            src_ref=ext.at[layer, pl.ds(rows, HALO)], dst_ref=ext.at[layer, pl.ds(0, HALO)],
            send_sem=hsem.at[layer, 0], recv_sem=hsem.at[layer, 1],
            device_id={"sp": sp + 1, "tp": tp}, device_id_type=MESH)

    barrier = pltpu.get_barrier_semaphore()

    def greet(device):
        pl.semaphore_signal(barrier, inc=1, device_id=device, device_id_type=MESH)

    greet({"sp": target[SIDE], "tp": tp})
    greet({"sp": target[CORE], "tp": tp})
    greet({"sp": sp, "tp": peer})
    pl.when(has_up)(lambda: greet({"sp": target[UP], "tp": tp}))
    pl.when(has_down)(lambda: greet({"sp": target[DOWN], "tp": tp}))
    pl.when(sp < n - 1)(lambda: greet({"sp": sp + 1, "tp": tp}))
    pl.when(sp > 0)(lambda: greet({"sp": sp - 1, "tp": tp}))

    lo = lax.broadcasted_iota(jnp.int32, (depth, LAYERS * depth), 0)
    hi = lax.broadcasted_iota(jnp.int32, (depth, LAYERS * depth), 1)
    clo = lax.broadcasted_iota(jnp.int32, (LAYERS * width, width), 1)
    chi = lax.broadcasted_iota(jnp.int32, (LAYERS * width, width), 0)

    for layer in range(LAYERS):
        pick = (hi == LAYERS * lo + layer).astype(jnp.float32).astype(jnp.bfloat16)
        for kind, ref in enumerate((v_ref, g_ref)):
            vg[layer * 2 + kind, sp] = jnp.dot(
                pick, ref[...], preferred_element_type=jnp.float32).astype(jnp.bfloat16)
        pick = (chi == LAYERS * clo + layer).astype(jnp.float32).astype(jnp.bfloat16)
        ob[layer, sp] = jnp.dot(
            o_ref[...], pick, preferred_element_type=jnp.float32).astype(jnp.bfloat16)
    xf[tp] = x_ref[...]

    @pl.when(sp == 0)
    def _():
        for layer in range(LAYERS):
            ext[layer, 0:HALO] = jnp.zeros((HALO, ch), jnp.float32)

    ends = [has_up, has_down, sp < n - 1, sp > 0]
    pl.semaphore_wait(barrier, 3 + sum(end.astype(jnp.int32) for end in ends))

    own(0, start)
    x_copy = to_peer(x_ref, xf.at[tp], (xsem.at[0], xsem.at[1]))
    x_copy.start()
    own(1, start)

    def normalise(source, layer):
        total = jnp.zeros((rows, 1), jnp.float32)
        for half in range(2):
            value = source[half].astype(jnp.float32)
            total = total + jnp.sum(value * value, axis=1, keepdims=True)
        scale = lax.rsqrt(total / D + EPS)
        for half in range(2):
            value = source[half].astype(jnp.float32)
            gain = ng_ref[layer : layer + 1, half * cols : (half + 1) * cols]
            nb[:, half * cols : (half + 1) * cols] = (value * scale * gain).astype(jnp.bfloat16)

    def glu(layer):
        value, gate = (
            jnp.dot(nb[...], vg[layer * 2 + kind].reshape(n * depth, ch),
                    preferred_element_type=jnp.float32) for kind in range(2))
        ext[layer, HALO:] = value * jax.nn.sigmoid(gate)
        pl.when(sp < n - 1)(lambda: halo(layer).start())

    def stat_copy(i):
        return to_peer(st.at[i], rst.at[i], (tsem.at[i, 0], tsem.at[i, 1]))

    def send_stats(i, first, second):
        lane = lax.broadcasted_iota(jnp.int32, (rows, 128), 1)
        turned = jnp.where(lane < 64, first, second).T
        st[i, 0:8] = turned[0:8]
        st[i, 8:16] = turned[64:72]
        stat_copy(i).start()

    def take_stats(i):
        stat_copy(i).wait_recv()
        both = st[i] + rst[i]
        turned = jnp.concatenate([both] * (128 // 16), axis=0).T
        return turned[:, 0:1], turned[:, 8:9]

    def conv(layer):
        tap_cols = pl.ds(pl.multiple_of(tp * ch, 128), ch)

        def chunk(r0):
            running = jnp.zeros((HALO, ch), jnp.float32)
            for k in range(KW):
                at = r0 + k + HALO - (KW - 1)
                running = running + taps_ref[layer, k : k + 1, tap_cols] * ext[layer, at : at + HALO]
            cv[r0 : r0 + HALO] = running

        for r0 in range(HALO, rows, HALO):
            chunk(r0)
        pl.when(sp > 0)(lambda: halo(layer).wait_recv())
        chunk(0)
        value = cv[...]
        send_stats(layer, jnp.sum(value, axis=1, keepdims=True),
                   jnp.sum(value * value, axis=1, keepdims=True))

    def activate(layer):
        first, second = take_stats(layer)
        mean = first / C
        var = second / C - mean * mean
        here = pl.ds(pl.multiple_of(tp * ch, 128), ch)
        v = (cv[...] - mean) * lax.rsqrt(var + EPS) * lng_ref[layer : layer + 1, here]
        v = v + lnb_ref[layer : layer + 1, here]
        act[...] = (v / (1.0 + jnp.exp(-v))).astype(jnp.bfloat16)

    pairs = n // 2
    half_pairs = pairs // 2

    def part_copy(layer, p):
        return to_peer(part.at[layer, p], rpart.at[layer, p], (psem.at[layer, 0, p], psem.at[layer, 1, p]))

    def project(layer, p):
        weights = jnp.concatenate([ob[layer, 2 * p], ob[layer, 2 * p + 1]], axis=1)
        part[layer, p] = jnp.dot(
            act[...], weights, preferred_element_type=jnp.float32).astype(jnp.bfloat16)

    def add_parts(layer, p):
        return part[layer, p].astype(jnp.float32) + rpart[layer, p].astype(jnp.float32)

    own(2, start)
    line(0, start, True)
    x_copy.wait_recv()
    normalise(xf, 0)
    own(3, start)
    line(1, start, True)
    across(0, start, True)
    own(4, start)
    line(2, start, True)
    across(1, start, True)
    own(5, start)
    other_core(0)
    other_core(1)
    glu(0)
    line(3, start, True)
    conv(0)
    across(2, start, True)
    activate(0)
    other_core(2)
    for p in range(pairs):
        project(0, p)
        part_copy(0, p).start()
    line(4, start, True)
    across(3, start, True)
    for p in range(pairs):
        part_copy(0, p).wait_recv()
        half, at = p // half_pairs, (p % half_pairs) * 2 * width
        here = xf[half, :, at : at + 2 * width].astype(jnp.float32)
        xn[half, :, at : at + 2 * width] = (here + add_parts(0, p)).astype(jnp.bfloat16)
    normalise(xn, 1)
    line(5, start, True)
    across(4, start, True)
    other_core(3)
    other_core(4)
    glu(1)
    conv(1)
    across(5, start, True)
    activate(1)
    other_core(5)
    for q in range(half_pairs):
        project(1, peer * half_pairs + q)
        part_copy(1, peer * half_pairs + q).start()
    for q in range(half_pairs):
        project(1, tp * half_pairs + q)
    squares = jnp.zeros((rows, 1), jnp.float32)
    for q in range(half_pairs):
        p = tp * half_pairs + q
        part_copy(1, p).wait_recv()
        at = q * 2 * width
        here = xn[tp, :, at : at + 2 * width].astype(jnp.float32)
        fresh = (here + add_parts(1, p)).astype(jnp.bfloat16)
        out_ref[:, at : at + 2 * width] = fresh
        fresh = fresh.astype(jnp.float32)
        squares = squares + jnp.sum(fresh * fresh, axis=1, keepdims=True)
    send_stats(LAYERS, squares, squares)
    total, _ = take_stats(LAYERS)
    gain = fg_ref[0:1, pl.ds(pl.multiple_of(tp * cols, 128), cols)]
    out_ref[...] = (
        out_ref[...].astype(jnp.float32) * lax.rsqrt(total / D + EPS) * gain).astype(jnp.bfloat16)

    for k in range(ITEMS):
        own(k, finish)
        line(k, finish, False)
        across(k, finish, False)
    x_copy.wait_send()
    for layer in range(LAYERS):
        pl.when(sp < n - 1)(lambda: halo(layer).wait_send())
    for i in range(LAYERS + 1):
        stat_copy(i).wait_send()
    for p in range(pairs):
        part_copy(0, p).wait_send()
    for q in range(half_pairs):
        part_copy(1, peer * half_pairs + q).wait_send()


def fused(n, stream, norm_gain, value_weight, gate_weight, conv_taps, ln_gain, ln_bias, out_weight, final_gain):
    rows, cols = stream.shape
    depth, ch = value_weight.shape[0] // LAYERS, value_weight.shape[1]
    width = out_weight.shape[1] // LAYERS
    bf16, f32 = jnp.bfloat16, jnp.float32
    dma = pltpu.SemaphoreType.DMA
    return pl.pallas_call(
        functools.partial(fused_kernel, n),
        out_shape=jax.ShapeDtypeStruct((rows, cols), bf16),
        in_specs=[pl.BlockSpec(memory_space=pltpu.VMEM)] * 9,
        out_specs=pl.BlockSpec(memory_space=pltpu.VMEM),
        scratch_shapes=[
            pltpu.VMEM((2 * LAYERS, n, depth, ch), bf16),
            pltpu.VMEM((LAYERS, n, ch, width), bf16),
            pltpu.VMEM((2, rows, cols), bf16),
            pltpu.VMEM((2, rows, cols), bf16),
            pltpu.VMEM((rows, 2 * cols), bf16),
            pltpu.VMEM((LAYERS, HALO + rows, ch), f32),
            pltpu.VMEM((rows, ch), f32),
            pltpu.VMEM((rows, ch), bf16),
            pltpu.VMEM((LAYERS, n // 2, rows, 2 * width), bf16),
            pltpu.VMEM((LAYERS, n // 2, rows, 2 * width), bf16),
            pltpu.VMEM((LAYERS + 1, 16, rows), f32),
            pltpu.VMEM((LAYERS + 1, 16, rows), f32),
            dma((ITEMS, 4, n)),
            dma((ITEMS, n)),
            dma((2,)),
            dma((LAYERS, 2)),
            dma((LAYERS + 1, 2)),
            dma((LAYERS, 2, n // 2)),
        ],
        compiler_params=pltpu.CompilerParams(collective_id=0, has_side_effects=True),
    )(stream, norm_gain, value_weight, gate_weight, conv_taps, ln_gain, ln_bias, out_weight,
      final_gain.reshape(1, -1))


def solution(mesh):
    placed = (P("sp", "tp"), P(), P("sp", "tp"), P("sp", "tp"), P(), P(), P(), P("tp", "sp"), P())
    n, n_tp = mesh.shape["sp"], mesh.shape["tp"]

    def step(*args):
        stream, out_weight = args[0], args[7]
        fits = n_tp == 2 and n % 4 == 0 and stream.shape[0] == 128 and out_weight.shape[1] == 128 * LAYERS
        return fused(n, *args) if fits else local(*args)

    return jax.shard_map(step, mesh=mesh, in_specs=placed, out_specs=P("sp", "tp"), check_vma=False)
```

```python
import functools

import jax
import jax.numpy as jnp
from jax import lax
from jax.experimental import pallas as pl
from jax.experimental.pallas import tpu as pltpu
from jax.sharding import PartitionSpec as P

D = 2048
C = 1024
KW = 31
LAYERS = 2


EPS = 1e-06


def from_behind(value, axis, steps):
    count = lax.axis_size(axis)
    first, last = (max(0, -steps), min(count, count - steps))
    return lax.ppermute(value, axis, [(source, source + steps) for source in range(first, last)])


def valid_conv(extended, tap_table):
    length = extended.shape[0] - (KW - 1)
    running = tap_table[0] * extended[0:length]
    for tap_index in range(1, KW):
        running = running + tap_table[tap_index] * extended[tap_index : tap_index + length]
    return running


def local(
    stream,
    norm_gain,
    value_weight,
    gate_weight,
    conv_taps,
    ln_gain,
    ln_bias,
    out_weight,
    final_gain,
):
    tokens_here = stream.shape[0]
    columns = stream.shape[1]
    channels = value_weight.shape[1]
    rim_rows = KW - 1
    tp_index = lax.axis_index("tp")
    my_taps = lax.dynamic_slice_in_dim(conv_taps, tp_index * channels, channels, 2)
    my_ln_gain = lax.dynamic_slice_in_dim(ln_gain, tp_index * channels, channels, 1)
    my_ln_bias = lax.dynamic_slice_in_dim(ln_bias, tp_index * channels, channels, 1)
    my_final = lax.dynamic_slice_in_dim(final_gain, tp_index * columns, columns, 0)
    value_all, gate_all, out_all = (
        lax.all_gather(value_weight, "sp", axis=0, tiled=True),
        lax.all_gather(gate_weight, "sp", axis=0, tiled=True),
        lax.all_gather(out_weight, "sp", axis=1, tiled=True),
    )
    value_all = value_all.reshape(D, LAYERS, channels)
    gate_all = gate_all.reshape(D, LAYERS, channels)
    out_all = out_all.reshape(channels, D, LAYERS)
    earlier = from_behind(stream[-LAYERS * rim_rows :], "sp", 1)
    current = jnp.concatenate([earlier, stream], axis=0)
    for layer_index in range(LAYERS):
        prefix = (LAYERS - layer_index) * rim_rows
        gathered = lax.all_gather(current, "tp", axis=1, tiled=True)
        gathered32 = gathered.astype(jnp.float32)
        scale = lax.rsqrt(jnp.sum(gathered32 * gathered32, axis=1, keepdims=True) / D + EPS)
        run_normed = (gathered32 * scale * norm_gain[layer_index]).astype(jnp.bfloat16)
        value_proj = jnp.dot(
            run_normed, value_all[:, layer_index], preferred_element_type=jnp.float32
        )
        gate_proj = jnp.dot(
            run_normed, gate_all[:, layer_index], preferred_element_type=jnp.float32
        )
        glu_out = value_proj * jax.nn.sigmoid(gate_proj)
        positions = (
            lax.axis_index("sp") * tokens_here - prefix + lax.iota(jnp.int32, current.shape[0])
        )
        extended = jnp.where((positions >= 0)[:, None], glu_out, 0.0)
        residual = current[rim_rows:].astype(jnp.float32)
        conv_out = valid_conv(extended, my_taps[layer_index])
        first_sums, square_sums = lax.psum(
            (jnp.sum(conv_out, axis=1), jnp.sum(conv_out * conv_out, axis=1)), "tp"
        )
        row_mean = (first_sums / C)[:, None]
        row_var = (square_sums / C)[:, None] - row_mean * row_mean
        run_active = jax.nn.silu(
            (conv_out - row_mean) * lax.rsqrt(row_var + EPS) * my_ln_gain[layer_index]
            + my_ln_bias[layer_index]
        ).astype(jnp.bfloat16)
        partial_value = jnp.dot(
            run_active, out_all[:, :, layer_index], preferred_element_type=jnp.float32
        )
        summed = lax.psum_scatter(
            partial_value.astype(jnp.bfloat16), "tp", scatter_dimension=1, tiled=True
        ).astype(jnp.float32)
        current = (residual + summed).astype(jnp.bfloat16)
    final32 = current.astype(jnp.float32)
    squares = lax.psum(jnp.sum(final32 * final32, axis=1), "tp")
    return (final32 * lax.rsqrt(squares[:, None] / D + EPS) * my_final).astype(jnp.bfloat16)


MESH = pl.DeviceIdType.MESH
HALO = 32
UP, DOWN, SIDE, CORE = range(4)
ITEMS = 3 * LAYERS
PAIRED = (0, 2, 4)


def fused_kernel(
    n, x_in, ng_in, v_in, g_in, taps_in, lng_in, lnb_in, o_in, fg_in, out_ref,
    x_ref, ng_ref, v_ref, g_ref, taps_ref, lng_ref, lnb_ref, o_ref, fg_ref, isem, vg, ob, xf, xn, nb, ext, cv, act, part, rpart, st, rst,
    ssem, rsem, xsem, hsem, tsem, psem,
):
    loads = [
        pltpu.make_async_copy(source, to, isem.at[i])
        for i, (source, to) in enumerate((
            (v_in, v_ref), (g_in, g_ref), (x_in, x_ref), (o_in, o_ref), (ng_in, ng_ref),
            (taps_in, taps_ref), (lng_in, lng_ref), (lnb_in, lnb_ref), (fg_in, fg_ref)))
    ]
    for load in loads:
        load.start()
    levels = n // 4
    sp = lax.axis_index("sp")
    tp = lax.axis_index("tp")
    z, y, core = sp // 4, (sp // 2) % 2, sp % 2
    peer = 1 - tp
    rows, cols = x_ref.shape
    depth = v_ref.shape[0] // LAYERS
    ch = v_ref.shape[1]
    width = o_ref.shape[1] // LAYERS
    has_up, has_down = z < levels - 1, z > 0
    even, odd = z % 2 == 0, z % 2 == 1
    target = {UP: sp + 4, DOWN: sp - 4, SIDE: sp + 2 - 4 * y, CORE: sp + 1 - 2 * core}

    def slot(k, src):
        layer, kind = divmod(k, 3)
        return ob.at[layer, src] if kind == 2 else vg.at[layer * 2 + kind, src]

    def copy(k, src, way):
        return pltpu.make_async_remote_copy(
            src_ref=slot(k, src), dst_ref=slot(k, src),
            send_sem=ssem.at[k, way, src], recv_sem=rsem.at[k, src],
            device_id={"sp": target[way], "tp": tp}, device_id_type=MESH)

    def index(zz, yy, cc):
        return (zz * 2 + yy) * 2 + cc

    def own(k, act_on):
        act_on(k, sp, SIDE)
        pl.when(has_up)(lambda: act_on(k, sp, UP))
        pl.when(has_down)(lambda: act_on(k, sp, DOWN))
        act_on(k, sp, CORE)

    def line(k, act_on, wait, steps=None):
        def one(src, way, more, to_side):
            if wait:
                copy(k, src, way).wait_recv()
            if to_side is not None:
                pl.when(to_side)(lambda: act_on(k, src, SIDE))
            else:
                act_on(k, src, SIDE)
            pl.when(more)(lambda: act_on(k, src, way))
            act_on(k, src, CORE)

        paired = k in PAIRED
        for d in steps or range(1, levels):
            near = paired and d == 1
            pl.when(z - d >= 0)(lambda: one(index(z - d, y, core), UP, has_up, even if near else None))
            pl.when(z + d < levels)(lambda: one(index(z + d, y, core), DOWN, has_down, odd if near else None))
            if d == 1:
                first = index(z, 1 - y, core)
                if wait:
                    copy(k, first, SIDE).wait_recv()
                if paired:
                    pl.when(even)(lambda: act_on(k, first, UP))
                    pl.when(odd)(lambda: act_on(k, first, DOWN))
                act_on(k, first, CORE)

    def across(k, act_on, wait, then=None):
        def one(zz):
            src = index(zz, 1 - y, core)
            if wait:
                copy(k, src, SIDE).wait_recv()
            act_on(k, src, CORE)
            if then is not None:
                then(zz, 1 - y)

        for d in range(1, levels):
            pl.when(z - d >= 0)(lambda: one(z - d))
            pl.when(z + d < levels)(lambda: one(z + d))

    def other_core(k):
        for zz in range(levels):
            for yy in range(2):
                copy(k, index(zz, yy, 1 - core), CORE).wait_recv()

    def start(k, src, way):
        copy(k, src, way).start()

    def finish(k, src, way):
        copy(k, src, way).wait_send()

    def to_peer(src, dst, sems):
        return pltpu.make_async_remote_copy(
            src_ref=src, dst_ref=dst, send_sem=sems[0], recv_sem=sems[1],
            device_id={"sp": sp, "tp": peer}, device_id_type=MESH)

    def halo(layer):
        return pltpu.make_async_remote_copy(
            src_ref=ext.at[layer, pl.ds(rows, HALO)], dst_ref=ext.at[layer, pl.ds(0, HALO)],
            send_sem=hsem.at[layer, 0], recv_sem=hsem.at[layer, 1],
            device_id={"sp": sp + 1, "tp": tp}, device_id_type=MESH)

    barrier = pltpu.get_barrier_semaphore()

    def greet(device):
        pl.semaphore_signal(barrier, inc=1, device_id=device, device_id_type=MESH)

    greet({"sp": target[SIDE], "tp": tp})
    greet({"sp": target[CORE], "tp": tp})
    greet({"sp": sp, "tp": peer})
    pl.when(has_up)(lambda: greet({"sp": target[UP], "tp": tp}))
    pl.when(has_down)(lambda: greet({"sp": target[DOWN], "tp": tp}))
    pl.when(sp < n - 1)(lambda: greet({"sp": sp + 1, "tp": tp}))
    pl.when(sp > 0)(lambda: greet({"sp": sp - 1, "tp": tp}))

    lo = lax.broadcasted_iota(jnp.int32, (depth, LAYERS * depth), 0)
    hi = lax.broadcasted_iota(jnp.int32, (depth, LAYERS * depth), 1)
    clo = lax.broadcasted_iota(jnp.int32, (LAYERS * width, width), 1)
    chi = lax.broadcasted_iota(jnp.int32, (LAYERS * width, width), 0)

    def pick_rows(kind, ref):
        for layer in range(LAYERS):
            pick = (hi == LAYERS * lo + layer).astype(jnp.float32).astype(jnp.bfloat16)
            vg[layer * 2 + kind, sp] = jnp.dot(
                pick, ref[...], preferred_element_type=jnp.float32).astype(jnp.bfloat16)

    def pick_columns():
        for layer in range(LAYERS):
            pick = (chi == LAYERS * clo + layer).astype(jnp.float32).astype(jnp.bfloat16)
            ob[layer, sp] = jnp.dot(
                o_ref[...], pick, preferred_element_type=jnp.float32).astype(jnp.bfloat16)

    loads[0].wait()
    pick_rows(0, v_ref)

    @pl.when(sp == 0)
    def _():
        for layer in range(LAYERS):
            ext[layer, 0:HALO] = jnp.zeros((HALO, ch), jnp.float32)

    ends = [has_up, has_down, sp < n - 1, sp > 0]
    pl.semaphore_wait(barrier, 3 + sum(end.astype(jnp.int32) for end in ends))

    own(0, start)
    loads[2].wait()
    x_copy = to_peer(x_ref, xf.at[tp], (xsem.at[0], xsem.at[1]))
    x_copy.start()
    loads[1].wait()
    pick_rows(1, g_ref)
    own(1, start)
    xf[tp] = x_ref[...]
    loads[3].wait()
    pick_columns()
    for load in loads[4:]:
        load.wait()

    def normalise(source, layer):
        total = jnp.zeros((rows, 1), jnp.float32)
        for half in range(2):
            value = source[half].astype(jnp.float32)
            total = total + jnp.sum(value * value, axis=1, keepdims=True)
        scale = lax.rsqrt(total / D + EPS)
        for half in range(2):
            value = source[half].astype(jnp.float32)
            gain = ng_ref[layer : layer + 1, half * cols : (half + 1) * cols]
            nb[:, half * cols : (half + 1) * cols] = (value * scale * gain).astype(jnp.bfloat16)

    def glu(layer):
        value, gate = (
            jnp.dot(nb[...], vg[layer * 2 + kind].reshape(n * depth, ch),
                    preferred_element_type=jnp.float32) for kind in range(2))
        ext[layer, HALO:] = value * jax.nn.sigmoid(gate)
        pl.when(sp < n - 1)(lambda: halo(layer).start())

    def stat_copy(i):
        return to_peer(st.at[i], rst.at[i], (tsem.at[i, 0], tsem.at[i, 1]))

    def send_stats(i, first, second):
        lane = lax.broadcasted_iota(jnp.int32, (rows, 128), 1)
        turned = jnp.where(lane < 64, first, second).T
        st[i, 0:8] = turned[0:8]
        st[i, 8:16] = turned[64:72]
        stat_copy(i).start()

    def take_stats(i):
        stat_copy(i).wait_recv()
        both = st[i] + rst[i]
        turned = jnp.concatenate([both] * (128 // 16), axis=0).T
        return turned[:, 0:1], turned[:, 8:9]

    def conv(layer):
        tap_cols = pl.ds(pl.multiple_of(tp * ch, 128), ch)

        def chunk(r0):
            running = jnp.zeros((HALO, ch), jnp.float32)
            for k in range(KW):
                at = r0 + k + HALO - (KW - 1)
                running = running + taps_ref[k, layer : layer + 1, tap_cols] * ext[layer, at : at + HALO]
            cv[r0 : r0 + HALO] = running

        for r0 in range(HALO, rows, HALO):
            chunk(r0)
        pl.when(sp > 0)(lambda: halo(layer).wait_recv())
        chunk(0)
        value = cv[...]
        send_stats(layer, jnp.sum(value, axis=1, keepdims=True),
                   jnp.sum(value * value, axis=1, keepdims=True))

    def activate(layer):
        first, second = take_stats(layer)
        mean = first / C
        var = second / C - mean * mean
        here = pl.ds(pl.multiple_of(tp * ch, 128), ch)
        v = (cv[...] - mean) * lax.rsqrt(var + EPS) * lng_ref[layer : layer + 1, here]
        v = v + lnb_ref[layer : layer + 1, here]
        act[...] = (v / (1.0 + jnp.exp(-v))).astype(jnp.bfloat16)

    pairs = n // 2
    half_pairs = pairs // 2

    def part_copy(layer, p):
        return to_peer(part.at[layer, p], rpart.at[layer, p], (psem.at[layer, 0, p], psem.at[layer, 1, p]))

    def project(layer, p):
        weights = jnp.concatenate([ob[layer, 2 * p], ob[layer, 2 * p + 1]], axis=1)
        part[layer, p] = jnp.dot(
            act[...], weights, preferred_element_type=jnp.float32).astype(jnp.bfloat16)

    def add_parts(layer, p):
        return part[layer, p].astype(jnp.float32) + rpart[layer, p].astype(jnp.float32)

    def project_last(zz, yy):
        p = zz * 2 + yy
        copy(ITEMS - 1, index(zz, yy, 1 - core), CORE).wait_recv()
        project(LAYERS - 1, p)
        pl.when(p // half_pairs == peer)(lambda: part_copy(LAYERS - 1, p).start())

    own(2, start)
    line(0, start, True)
    x_copy.wait_recv()
    normalise(xf, 0)
    own(3, start)
    line(1, start, True)
    across(0, start, True)
    own(4, start)
    near, far = range(1, levels - 1), range(levels - 1, levels)
    line(2, start, True, near)
    across(1, start, True)
    own(5, start)
    other_core(0)
    other_core(1)
    glu(0)
    line(2, start, True, far)
    line(3, start, True, near)
    conv(0)
    line(3, start, True, far)
    across(2, start, True)
    activate(0)
    other_core(2)
    for p in range(pairs):
        project(0, p)
        part_copy(0, p).start()
        if p == half_pairs:
            line(4, start, True, near)
    line(4, start, True, far)
    across(3, start, True)
    line(5, start, True)
    for p in range(pairs):
        part_copy(0, p).wait_recv()
        half, at = p // half_pairs, (p % half_pairs) * 2 * width
        here = xf[half, :, at : at + 2 * width].astype(jnp.float32)
        xn[half, :, at : at + 2 * width] = (here + add_parts(0, p)).astype(jnp.bfloat16)
    normalise(xn, 1)
    across(4, start, True)
    other_core(3)
    other_core(4)
    glu(1)
    conv(1)
    activate(1)
    project_last(z, y)
    for d in range(1, levels):
        pl.when(z - d >= 0)(lambda: project_last(z - d, y))
        pl.when(z + d < levels)(lambda: project_last(z + d, y))
    project_last(z, 1 - y)
    across(5, start, True, project_last)
    squares = jnp.zeros((rows, 1), jnp.float32)
    for q in range(half_pairs):
        p = tp * half_pairs + q
        part_copy(1, p).wait_recv()
        at = q * 2 * width
        here = xn[tp, :, at : at + 2 * width].astype(jnp.float32)
        fresh = (here + add_parts(1, p)).astype(jnp.bfloat16)
        out_ref[:, at : at + 2 * width] = fresh
        fresh = fresh.astype(jnp.float32)
        squares = squares + jnp.sum(fresh * fresh, axis=1, keepdims=True)
    send_stats(LAYERS, squares, squares)
    total, _ = take_stats(LAYERS)
    gain = fg_ref[0:1, pl.ds(pl.multiple_of(tp * cols, 128), cols)]
    out_ref[...] = (
        out_ref[...].astype(jnp.float32) * lax.rsqrt(total / D + EPS) * gain).astype(jnp.bfloat16)

    for k in range(ITEMS):
        own(k, finish)
        line(k, finish, False)
        across(k, finish, False)
    x_copy.wait_send()
    for layer in range(LAYERS):
        pl.when(sp < n - 1)(lambda: halo(layer).wait_send())
    for i in range(LAYERS + 1):
        stat_copy(i).wait_send()
    for p in range(pairs):
        part_copy(0, p).wait_send()
    for q in range(half_pairs):
        part_copy(1, peer * half_pairs + q).wait_send()


def fused(n, stream, norm_gain, value_weight, gate_weight, conv_taps, ln_gain, ln_bias, out_weight, final_gain):
    rows, cols = stream.shape
    depth, ch = value_weight.shape[0] // LAYERS, value_weight.shape[1]
    width = out_weight.shape[1] // LAYERS
    bf16, f32 = jnp.bfloat16, jnp.float32
    dma = pltpu.SemaphoreType.DMA
    arrays = (stream, norm_gain, value_weight, gate_weight, conv_taps.transpose(1, 0, 2),
              ln_gain, ln_bias, out_weight, final_gain.reshape(1, -1))
    return pl.pallas_call(
        functools.partial(fused_kernel, n),
        out_shape=jax.ShapeDtypeStruct((rows, cols), bf16),
        in_specs=[pl.BlockSpec(memory_space=pl.ANY)] * 9,
        out_specs=pl.BlockSpec(memory_space=pltpu.VMEM),
        scratch_shapes=[pltpu.VMEM(array.shape, array.dtype) for array in arrays] + [
            dma((len(arrays),)),
            pltpu.VMEM((2 * LAYERS, n, depth, ch), bf16),
            pltpu.VMEM((LAYERS, n, ch, width), bf16),
            pltpu.VMEM((2, rows, cols), bf16),
            pltpu.VMEM((2, rows, cols), bf16),
            pltpu.VMEM((rows, 2 * cols), bf16),
            pltpu.VMEM((LAYERS, HALO + rows, ch), f32),
            pltpu.VMEM((rows, ch), f32),
            pltpu.VMEM((rows, ch), bf16),
            pltpu.VMEM((LAYERS, n // 2, rows, 2 * width), bf16),
            pltpu.VMEM((LAYERS, n // 2, rows, 2 * width), bf16),
            pltpu.VMEM((LAYERS + 1, 16, rows), f32),
            pltpu.VMEM((LAYERS + 1, 16, rows), f32),
            dma((ITEMS, 4, n)),
            dma((ITEMS, n)),
            dma((2,)),
            dma((LAYERS, 2)),
            dma((LAYERS + 1, 2)),
            dma((LAYERS, 2, n // 2)),
        ],
        compiler_params=pltpu.CompilerParams(collective_id=0, has_side_effects=True),
    )(*arrays)


def solution(mesh):
    placed = (P("sp", "tp"), P(), P("sp", "tp"), P("sp", "tp"), P(), P(), P(), P("tp", "sp"), P())
    n, n_tp = mesh.shape["sp"], mesh.shape["tp"]

    def step(*args):
        stream, out_weight = args[0], args[7]
        fits = n_tp == 2 and n % 8 == 0 and stream.shape[0] == 128 and out_weight.shape[1] == 128 * LAYERS
        return fused(n, *args) if fits else local(*args)

    return jax.shard_map(step, mesh=mesh, in_specs=placed, out_specs=P("sp", "tp"), check_vma=False)
```
